32 devices in a mesh: ep: 8 (over z, x), tp: 4 (over y, core).
Axes of the slice: x: 2, y: 2, z: 4, core: 2. Of those that a mesh axis runs over, the one named last changes fastest.
Arguments:
- mixer_input_rows: bfloat16 [1024, 2048], P('ep'), may hold values from -6 to 6
- mix_gain: float32 [2048], replicated, may hold values from 0.1 to 1.9
- w_recept: bfloat16 [2048, 1024], P(None, 'tp'), may hold values from -0.125 to 0.125
- w_key: bfloat16 [2048, 1024], P(None, 'tp'), may hold values from -0.125 to 0.125
- w_value: bfloat16 [2048, 1024], P(None, 'tp'), may hold values from -0.125 to 0.125
- lowered_map_factor: bfloat16 [2048, 64], replicated, may hold values from -0.125 to 0.125
- decay_up: bfloat16 [64, 1024], P(None, 'tp'), may hold values from -0.75 to 0.75
- rate_up: bfloat16 [64, 1024], P(None, 'tp'), may hold values from -0.75 to 0.75
- decay_base: float32 [1024], P('tp'), may hold values from -13 to -2
- rate_base: float32 [1024], P('tp'), may hold values from -9 to 1
- decay_shift: float32 [1024, 16], P('ep', 'tp'), may hold values from -0.7 to 0, as said below
- out_gain: float32 [1024], P('tp'), may hold values from 0.1 to 1.9
- w_output: bfloat16 [1024, 2048], P('tp'), may hold values from -0.1875 to 0.1875
- moe_rows: bfloat16 [1024, 2048], P('ep'), may hold values from -6 to 6
- moe_gain: float32 [2048], replicated, may hold values from 0.1 to 1.9
- routes: int32 [1024, 2], P('ep'), may hold values from 0 to 7, all different within a row; in each aligned block of 128 rows (0 to 127, 128 to 255, ...) at most 64 rows name the same one
- route_weight: float32 [1024, 2], P('ep'), may hold values from 0.1 to 1
- exp_gate: bfloat16 [8, 2048, 4096], P('ep', None, 'tp'), may hold values from -0.125 to 0.125
- exp_up: bfloat16 [8, 2048, 4096], P('ep', None, 'tp'), may hold values from -0.125 to 0.125
- exp_down: bfloat16 [8, 4096, 2048], P('ep', 'tp'), may hold values from -0.125 to 0.125
Outputs:
- mix_out: bfloat16 [1024, 2048], P(('ep', 'tp'))
- moe_out: bfloat16 [1024, 2048], P('ep', 'tp')
The draws below stay inside these ranges and needn't reach their ends.
Inputs may be any that keep to these rules, and one draw needn't show every extreme that they name: `routes`: in each aligned block of 128 rows no expert is named more than 64 times, and in some block one expert is named exactly 64 times; the two entries of a row differ. `decay_shift`: at most zero.
All inputs are finite; a program needn't handle non-finite values.
Results may differ from the reference program's by a relative error of at most 0.02.
Values may be sent and summed in bfloat16 or wider, within the bound.
A program may use at most 64 MiB of HBM per device.

```python
import math
from functools import partial
import jax
import jax.numpy as jnp
import numpy as np
from jax import lax

D = 2048
HEADS = 16
HEAD_DIM = 64
RANK = 64
EXP_HIDDEN = 4096
MIX_TOK = 128
MOE_TOK = 128
CHANNELS = 1024
SEQ_ITEMS_FIRST = 1024
MOE_TOKENS = 1024
EXPERTS = 8
SLOTS = 64
N_EP = 8
N_TP = 4


def head_groups(key):
    fast_count = max(1, HEADS // 4)
    middle_count = max(1, HEADS // 4)
    shuffled = jax.random.permutation(jax.random.fold_in(key, 101), HEADS)
    group_ids = jnp.where(shuffled < fast_count, 0, jnp.where(shuffled < fast_count + middle_count, 1, 2))
    return jnp.repeat(group_ids, HEAD_DIM)


def draw_decay_base(key, part):
    group_ids = head_groups(key)
    spread = jax.random.uniform(jax.random.fold_in(key, 1), (CHANNELS,), jnp.float32)
    return jnp.where(group_ids == 0, -3.5 + 1.5 * spread, -13.0 + 2.5 * spread)


def draw_rate_base(key, part):
    group_ids = head_groups(key)
    spread = jax.random.uniform(jax.random.fold_in(key, 2), (CHANNELS,), jnp.float32)
    fast_level = -1.5 + 2.5 * spread
    middle_level = -4.0 + 3.0 * spread
    slow_level = -9.0 + 2.0 * spread
    return jnp.where(group_ids == 0, fast_level, jnp.where(group_ids == 1, middle_level, slow_level))


def draw_decay_shift(key, part):
    low_level = 2e-05
    high_level = 0.0002
    blocks = SEQ_ITEMS_FIRST // MIX_TOK
    level_draw = jax.random.uniform(jax.random.fold_in(key, 3), (blocks, HEADS), jnp.float32)
    hierarchy_tiers = jnp.exp(jnp.log(low_level) + (jnp.log(high_level) - jnp.log(low_level)) * level_draw)
    hierarchy_tiers = jnp.repeat(hierarchy_tiers, MIX_TOK, axis=0)
    spike_offsets = jax.random.randint(jax.random.fold_in(key, 5), (3,), 0, SEQ_ITEMS_FIRST)
    entry_offsets = jnp.arange(SEQ_ITEMS_FIRST)
    spike_entry_tile = jnp.any(entry_offsets[:, None] == spike_offsets[None, :], axis=1)
    prefix_heights = jax.random.uniform(jax.random.fold_in(key, 7), (SEQ_ITEMS_FIRST, HEADS), jnp.float32, 0.22, 0.69)
    return -hierarchy_tiers - jnp.where(spike_entry_tile[:, None], prefix_heights, 0.0)


def spiked(result, own_key, source, target, blocks, factor):
    def block_of(dim):
        return (jnp.arange(result.shape[dim]) // (result.shape[dim] // blocks)).reshape((-1,) + (1,) * (result.ndim - 1 - dim))

    first = jax.random.permutation(own_key, blocks)[block_of(target)]
    far = (block_of(target) + blocks // 2) % blocks
    return jnp.where((block_of(source) == first) | (block_of(source) == far), factor * result, result)


def shard_levels(stream_key, extent, shards, smallest, top_value):
    gain, own = 1.0, jax.random.fold_in(stream_key, 6)
    for dim, blocks in shards:
        steps = jnp.exp(jax.random.uniform(jax.random.fold_in(own, dim), (blocks,), jnp.float32, smallest / len(shards), top_value / len(shards)))
        gain = gain * jnp.repeat(steps, extent[dim] // blocks).reshape([-1 if axis == dim else 1 for axis in range(len(extent))])
    return gain


def deal_out(key, own, number, rows, amount, top, most, skew):
    order = jax.random.permutation(key, amount)
    crowded, usual = shares(amount, rows * top, most, skew, True), shares(amount, rows * top, most, skew, False)
    places = jnp.arange(amount)

    def named(sizes, rotation):
        used = int((sizes > 0).sum())
        fixed = max(1, used // 4)
        moved = fixed + (places - fixed + rotation * (used - fixed)) % max(1, amount - fixed)
        return jnp.zeros((amount,), jnp.int32).at[order[jnp.where(places < fixed, places, moved)]].set(jnp.asarray(sizes, jnp.int32))

    sizes = jnp.where(number % 4 == 0, named(crowded, number // 4), named(usual, number - number // 4 - 1))
    mixed = jax.random.permutation(jax.random.fold_in(own, 3), amount)
    donor, sink = mixed[0:amount // 2 * 2:2], mixed[1:amount // 2 * 2:2]
    room = jnp.minimum(sizes[donor] - 1, most - sizes[sink]) // 2
    room = jnp.where((donor == order[0]) | (sink == order[0]) | (sizes[sink] == 0), 0, jnp.maximum(room, 0))
    moved = jax.random.randint(jax.random.fold_in(own, 4), (amount // 2,), 0, 1 << 20) % (room + 1)
    sizes = sizes.at[donor].add(-moved).at[sink].add(moved)
    labels = jnp.searchsorted(jnp.cumsum(sizes), jnp.arange(rows * top), side="right").astype(jnp.int32)
    grid = labels.reshape(top, rows).T
    grid = grid[jax.random.permutation(jax.random.fold_in(own, 1), rows)]
    rotation = jax.random.randint(jax.random.fold_in(own, 2), (rows, 1), 0, top)
    return jnp.take_along_axis(grid, (jnp.arange(top)[None, :] + rotation) % top, axis=1)


def shares(count, total, most, skew, full):
    loads = [(1 << 20) // math.isqrt(grade ** skew) + 1 for grade in range(1, count + 1)]
    largest = most if full else min(most, max(-(-total // count), total * loads[0] // sum(loads)))
    least = 1 if total - largest >= count - 1 else 0
    given, rest = [largest] + [least] * (count - 1), total - largest - least * (count - 1)
    while rest > 0:
        free = [i for i in range(1, count) if given[i] < largest] or [i for i in range(1, count) if given[i] < most]
        whole, budget = sum([loads[i] for i in free]), rest
        for i in free:
            more = min(most - given[i], max(1, budget * loads[i] // whole), rest)
            given[i] = given[i] + more
            rest = rest - more
    return np.array(given)


def noise(own_key, dims, width, reach, cuts=(), kind=jnp.bfloat16):
    array = jax.random.normal(own_key, dims, jnp.float32) * width
    if len(cuts) > 0:
        array = shard_levels(own_key, dims, cuts, -0.22, 0.18) * array
    return jnp.clip(array, min=-reach, max=reach).astype(kind)


def gaussian_with(stream_key, shape, width, reach, shards, heavy, held_as=jnp.bfloat16):
    result = width * jax.random.normal(stream_key, shape, jnp.float32)
    if shards:
        result = result * shard_levels(stream_key, shape, shards, -0.22, 0.18)
    return jnp.clip(spiked(result, jax.random.fold_in(stream_key, 3), *heavy), -reach, reach).astype(held_as)


def setup_inputs(seed: int = 0) -> dict:
    arg_keys = jax.random.split(jax.random.key(seed), 21)
    mixer_input_rows = noise(arg_keys[0], (SEQ_ITEMS_FIRST, D), 1.0, 6.0, ((0, 8),))
    mix_gain = jnp.clip(1.0 + 0.18 * jax.random.normal(arg_keys[1], (D,), jnp.float32), 0.1, 1.9)
    w_recept = noise(arg_keys[2], (D, CHANNELS), D ** -0.5, 0.125, ((1, 4),))
    w_key = noise(arg_keys[3], (D, CHANNELS), D ** -0.5, 0.125, ((1, 4),))
    w_value = noise(arg_keys[4], (D, CHANNELS), D ** -0.5, 0.125, ((1, 4),))
    lowered_map_factor = noise(arg_keys[5], (D, RANK), D ** -0.5, 0.125)
    decay_up = noise(arg_keys[6], (RANK, CHANNELS), RANK ** -0.5, 0.75, ((1, 4),))
    rate_up = noise(arg_keys[7], (RANK, CHANNELS), RANK ** -0.5, 0.75, ((1, 4),))
    decay_base = draw_decay_base(jax.random.fold_in(arg_keys[20], 71), 0)
    rate_base = draw_rate_base(jax.random.fold_in(arg_keys[20], 71), 0)
    decay_shift = draw_decay_shift(jax.random.fold_in(arg_keys[20], 71), 0)
    out_gain = jnp.clip(1.0 + 0.18 * jax.random.normal(arg_keys[11], (CHANNELS,), jnp.float32), 0.1, 1.9)
    w_output = noise(arg_keys[12], (CHANNELS, D), CHANNELS ** -0.5, 0.1875, ((0, 4),))
    moe_rows = noise(arg_keys[13], (MOE_TOKENS, D), 1.0, 6.0, ((0, 8),))
    moe_gain = jnp.clip(1.0 + 0.18 * jax.random.normal(arg_keys[14], (D,), jnp.float32), 0.1, 1.9)
    routes_keys = jax.random.split(jax.random.fold_in(arg_keys[15], 1), MOE_TOKENS // MOE_TOK)
    routes_turns = jax.random.permutation(jax.random.fold_in(arg_keys[15], 3), MOE_TOKENS // MOE_TOK)
    routes = jax.vmap(lambda own, number: deal_out(jax.random.fold_in(arg_keys[15], 2), own, number, MOE_TOK, EXPERTS, 2, SLOTS, 2))(routes_keys, routes_turns).reshape((MOE_TOKENS, 2))
    route_weight = jnp.clip(0.1 + 0.9 * jax.random.uniform(arg_keys[16], (MOE_TOKENS, 2), jnp.float32) ** shard_levels(arg_keys[16], (MOE_TOKENS, 2), ((0, 8),), -0.2, 0.2), 0.1, 1.0)
    exp_gate = noise(arg_keys[17], (EXPERTS, D, EXP_HIDDEN), D ** -0.5, 0.125, ((0, 8), (2, 4)))
    exp_up = noise(arg_keys[18], (EXPERTS, D, EXP_HIDDEN), D ** -0.5, 0.125, ((0, 8), (2, 4)))
    exp_down = gaussian_with(arg_keys[19], (EXPERTS, EXP_HIDDEN, D), EXP_HIDDEN ** -0.5, 0.125, ((0, 8), (1, 4)), (1, 2, 4, 2.0))
    return {"mixer_input_rows": mixer_input_rows, "mix_gain": mix_gain, "w_recept": w_recept, "w_key": w_key, "w_value": w_value, "lowered_map_factor": lowered_map_factor, "decay_up": decay_up, "rate_up": rate_up, "decay_base": decay_base, "rate_base": rate_base, "decay_shift": decay_shift, "out_gain": out_gain, "w_output": w_output, "moe_rows": moe_rows, "moe_gain": moe_gain, "routes": routes, "route_weight": route_weight, "exp_gate": exp_gate, "exp_up": exp_up, "exp_down": exp_down}


HIGHEST = lax.Precision.HIGHEST
DECAY_SCALE = math.exp(-0.5)

def row_norm(row_block, gain_vector):
    entries = row_block.astype(jnp.float32)
    factor = lax.rsqrt(lax.optimization_barrier(jnp.mean(entries * entries, axis=-1, keepdims=True)) + 1e-06)
    return (entries * factor * gain_vector.astype(jnp.float32)).astype(jnp.bfloat16)

def block_sum(left_side, right_side, blocks):
    block_width = left_side.shape[1] // blocks

    def accumulate(running, position):
        start_at = (position * block_width).astype(jnp.int32)
        left_part = lax.dynamic_slice_in_dim(left_side, start_at, block_width, 1)
        right_part = lax.dynamic_slice_in_dim(right_side, start_at, block_width, 0)
        product = jnp.dot(left_part, right_part, preferred_element_type=jnp.float32)
        rounded = lax.optimization_barrier(product.astype(jnp.bfloat16))
        return (running + rounded.astype(jnp.float32), None)
    start_sum = jnp.zeros((left_side.shape[0], right_side.shape[1]), jnp.float32)
    running, _ = lax.scan(accumulate, start_sum, jnp.arange(blocks, dtype=jnp.int32))
    return running.astype(jnp.bfloat16)

def route_tables(route_rows, weight_rows, expert_count, slot_count):
    route_list = route_rows.reshape(-1)
    onehot = (route_list[:, None] == jnp.arange(expert_count, dtype=jnp.int32)[None, :]).astype(jnp.int32)
    slot_index = lax.optimization_barrier(jnp.sum((jnp.cumsum(onehot, axis=0) - onehot) * onehot, axis=1))
    target = (route_list * slot_count + slot_index).reshape(route_rows.shape)
    columns = jnp.arange(expert_count * slot_count, dtype=jnp.int32)
    matches = target[:, :, None] == columns[None, None, :]
    placing = lax.optimization_barrier(jnp.sum(matches.astype(jnp.int32), axis=1)).astype(jnp.bfloat16)
    rounded = weight_rows.astype(jnp.bfloat16)
    weighing = lax.optimization_barrier(jnp.sum(jnp.where(matches, rounded[:, :, None], jnp.zeros((), jnp.bfloat16)), axis=1))
    return (placing, weighing.astype(jnp.bfloat16))

def mixer(mixer_input_rows, mix_gain, w_recept, w_key, w_value, lowered_map_factor, decay_up, rate_up, decay_base, rate_base, decay_shift, out_gain, w_output):
    normed_input = row_norm(mixer_input_rows, mix_gain)

    def heads_of(weight):
        product = jnp.dot(normed_input, weight, preferred_element_type=jnp.float32)
        rounded = lax.optimization_barrier(product.astype(jnp.bfloat16))
        return rounded.astype(jnp.float32).reshape(SEQ_ITEMS_FIRST, HEADS, HEAD_DIM)
    recept_heads = heads_of(w_recept)
    key_heads = heads_of(w_key)
    value_heads = heads_of(w_value)
    lowrank = jnp.tanh(jnp.dot(normed_input, lowered_map_factor, preferred_element_type=jnp.float32)).astype(jnp.bfloat16)
    decay_pre = decay_base + jnp.dot(lowrank, decay_up, preferred_element_type=jnp.float32)
    log_decay = -DECAY_SCALE * jax.nn.sigmoid(decay_pre) + jnp.repeat(decay_shift, HEAD_DIM, axis=1)
    learn_rate = jax.nn.sigmoid(rate_base + jnp.dot(lowrank, rate_up, preferred_element_type=jnp.float32))
    decay_rate = jnp.exp(log_decay).reshape(SEQ_ITEMS_FIRST, HEADS, HEAD_DIM)
    learn_rate = learn_rate.reshape(SEQ_ITEMS_FIRST, HEADS, HEAD_DIM)
    unit_key = key_heads * lax.rsqrt(lax.optimization_barrier(jnp.sum(key_heads * key_heads, axis=-1, keepdims=True)) + 1e-06)

    def advance(memory, inputs):
        decay_row, unit_row, learn_row, key_row, value_row, recept_row = inputs
        along_key = jnp.einsum('hij,hj->hi', memory, unit_row, precision=HIGHEST)
        memory = memory * decay_row[:, None, :] - along_key[:, :, None] * (unit_row * learn_row)[:, None, :] + value_row[:, :, None] * key_row[:, None, :]
        return (memory, jnp.einsum('hij,hj->hi', memory, recept_row, precision=HIGHEST))
    start_state = jnp.zeros((HEADS, HEAD_DIM, HEAD_DIM), jnp.float32)
    sequence = (decay_rate, unit_key, learn_rate, key_heads, value_heads, recept_heads)
    _, forward_out = lax.scan(advance, start_state, sequence)
    _, backward_out = lax.scan(advance, start_state, sequence, reverse=True)
    mixed_out = forward_out + backward_out
    centre = mixed_out - lax.optimization_barrier(jnp.mean(mixed_out, axis=-1, keepdims=True))
    scaled = centre * lax.rsqrt(lax.optimization_barrier(jnp.mean(centre * centre, axis=-1, keepdims=True)) + 1e-05)
    grouped = (scaled * out_gain.reshape(HEADS, HEAD_DIM)).astype(jnp.bfloat16).reshape(SEQ_ITEMS_FIRST, CHANNELS)
    return block_sum(grouped, w_output, N_TP)

def fill_slots(placing_group, rows_group):
    product = lax.dot_general(placing_group, rows_group, (((0,), (0,)), ((), ())), preferred_element_type=jnp.float32)
    return product.astype(jnp.bfloat16)

def combine_group(weighing_group, result_group):
    return jnp.dot(weighing_group, result_group, preferred_element_type=jnp.float32).astype(jnp.bfloat16)

def experts_layer(moe_rows, moe_gain, routes, route_weight, exp_gate, exp_up, exp_down):
    moe_normed = row_norm(moe_rows, moe_gain)
    group_rows = moe_normed.reshape(N_EP, MOE_TOK, D)
    group_routes = routes.reshape(N_EP, MOE_TOK, 2)
    group_weights = route_weight.reshape(N_EP, MOE_TOK, 2)
    tables = jax.vmap(partial(route_tables, expert_count=EXPERTS, slot_count=SLOTS))
    placing, weighing = tables(group_routes, group_weights)
    buffers = jax.vmap(fill_slots)(placing, group_rows).reshape(N_EP, EXPERTS, SLOTS, D)

    def run_expert(expert_index):
        slot_rows = lax.dynamic_index_in_dim(buffers, expert_index, 1, keepdims=False).reshape(N_EP * SLOTS, D)
        gate_weight = lax.dynamic_index_in_dim(exp_gate, expert_index, 0, keepdims=False)
        up_weight = lax.dynamic_index_in_dim(exp_up, expert_index, 0, keepdims=False)
        down_weight = lax.dynamic_index_in_dim(exp_down, expert_index, 0, keepdims=False)
        gate_part = jnp.dot(slot_rows, gate_weight, preferred_element_type=jnp.float32)
        up_part = jnp.dot(slot_rows, up_weight, preferred_element_type=jnp.float32)
        hidden = (jax.nn.silu(gate_part) * up_part).astype(jnp.bfloat16)
        return block_sum(hidden, down_weight, N_TP)
    results = lax.map(run_expert, jnp.arange(EXPERTS, dtype=jnp.int32))
    results = jnp.swapaxes(results.reshape(EXPERTS, N_EP, SLOTS, D), 0, 1).reshape(N_EP, EXPERTS * SLOTS, D)
    combined = jax.vmap(combine_group)(weighing, results)
    return combined.reshape(MOE_TOKENS, D)

def reference(mixer_input_rows, mix_gain, w_recept, w_key, w_value, lowered_map_factor, decay_up, rate_up, decay_base, rate_base, decay_shift, out_gain, w_output, moe_rows, moe_gain, routes, route_weight, exp_gate, exp_up, exp_down):
    mix_out = mixer(mixer_input_rows, mix_gain, w_recept, w_key, w_value, lowered_map_factor, decay_up, rate_up, decay_base, rate_base, decay_shift, out_gain, w_output)
    moe_out = experts_layer(moe_rows, moe_gain, routes, route_weight, exp_gate, exp_up, exp_down)
    return (mix_out, moe_out)
```

```python
import functools
import math

import jax
import jax.numpy as jnp
from jax import lax
from jax.experimental import pallas as pl
from jax.experimental.pallas import tpu as pltpu
from jax.sharding import PartitionSpec as P

HIGHEST = lax.Precision.HIGHEST
DECAY_SCALE = math.exp(-0.5)


def row_norm(row_block, gain_vector):
    entries = row_block.astype(jnp.float32)
    factor = lax.rsqrt(jnp.mean(entries * entries, axis=-1, keepdims=True) + 1e-06)
    return (entries * factor * gain_vector).astype(jnp.bfloat16)


F32 = jnp.float32
BF16 = jnp.bfloat16
CHUNK = 64


def mul(left, right, left_dim=1, right_dim=0):
    return lax.dot_general(
        left.astype(BF16),
        right.astype(BF16),
        (((left_dim,), (right_dim,)), ((), ())),
        preferred_element_type=F32,
    )


def local_kernel(
    heads,
    width,
    rows_ref,
    gain_ref,
    recept_ref,
    key_ref,
    value_ref,
    low_ref,
    decay_up_ref,
    rate_up_ref,
    decay_base_ref,
    rate_base_ref,
    shift_ref,
    totals_ref,
    read_ref,
    own_ref,
):
    tokens = rows_ref.shape[0]
    chunk = min(CHUNK, tokens)
    chunks = tokens // chunk
    normed = row_norm(rows_ref[...], gain_ref[...])
    recept = jnp.dot(normed, recept_ref[...], preferred_element_type=F32).astype(BF16)
    keys = jnp.dot(normed, key_ref[...], preferred_element_type=F32).astype(BF16).astype(F32)
    values = jnp.dot(normed, value_ref[...], preferred_element_type=F32).astype(BF16)
    recept = recept.astype(F32)
    low = jnp.tanh(jnp.dot(normed, low_ref[...], preferred_element_type=F32)).astype(BF16)
    decay_pre = decay_base_ref[...] + jnp.dot(low, decay_up_ref[...], preferred_element_type=F32)
    rate = jax.nn.sigmoid(
        rate_base_ref[...] + jnp.dot(low, rate_up_ref[...], preferred_element_type=F32)
    )
    shift = shift_ref[...]
    shift_wide = jnp.concatenate(
        [jnp.broadcast_to(shift[:, h : h + 1], (tokens, width)) for h in range(heads)], axis=1
    )
    log_decay = -DECAY_SCALE * jax.nn.sigmoid(decay_pre) + shift_wide

    row = lax.broadcasted_iota(jnp.int32, (tokens, tokens), 0)
    col = lax.broadcasted_iota(jnp.int32, (tokens, tokens), 1)
    same = (row // chunk) == (col // chunk)
    lower = jnp.where(same & (row >= col), 1.0, 0.0).astype(F32)
    running = jnp.dot(lower, log_decay, precision=HIGHEST, preferred_element_type=F32)
    ends = [running[(c + 1) * chunk - 1 : (c + 1) * chunk, :] for c in range(chunks)]
    total = jnp.concatenate(
        [jnp.broadcast_to(end, (chunk, end.shape[1])) for end in ends], axis=0
    )
    half = 0.5 * total
    squares = keys * keys
    unit = jnp.concatenate(
        [
            keys[:, h * width : (h + 1) * width]
            * lax.rsqrt(
                jnp.sum(squares[:, h * width : (h + 1) * width], axis=-1, keepdims=True) + 1e-06
            )
            for h in range(heads)
        ],
        axis=1,
    )
    learned = unit * rate
    sides = []
    for reverse in (False, True):
        upto = total - running + log_decay if reverse else running
        before = upto - log_decay
        up_scale = jnp.exp(upto - half)
        down_scale = jnp.exp(half - upto)
        tail = jnp.exp(total - upto)
        sides.append(
            (
                (unit * jnp.exp(before - half)).astype(BF16),
                (recept * up_scale).astype(BF16),
                (learned * down_scale).astype(BF16),
                (keys * down_scale).astype(BF16),
                unit * jnp.exp(before),
                recept * jnp.exp(upto),
                (learned * tail).astype(BF16),
                (keys * tail).astype(BF16),
            )
        )
    problems = [(h, d) for h in range(heads) for d in range(2)]
    products, inverses, lowers = {}, {}, {}
    for p in problems:
        h, d = p
        cut = slice(h * width, (h + 1) * width)
        a_side, q_side, b_side, c_side = [side[:, cut] for side in sides[d][:4]]
        pair = mul(
            jnp.concatenate([a_side, q_side], axis=0),
            jnp.concatenate([b_side, c_side], axis=0),
            1,
            1,
        )
        strict = same & ((row < col) if d else (row > col))
        whole = same & ((row <= col) if d else (row >= col))
        a_b = jnp.where(strict, pair[:tokens, :tokens], 0.0)
        a_c = jnp.where(strict, pair[:tokens, tokens:], 0.0)
        q_b = jnp.where(whole, pair[tokens:, :tokens], 0.0)
        q_c = jnp.where(whole, pair[tokens:, tokens:], 0.0)
        by_value = mul(jnp.concatenate([a_c, q_c], axis=0), values[:, cut])
        products[p] = (by_value[:tokens], by_value[tokens:], q_b)
        lowers[p] = a_b.astype(BF16)
        near = (row // 2) == (col // 2)
        inverses[p] = jnp.where(row == col, 1.0, jnp.where(near, -a_b, 0.0))
    size = 2
    while size < chunk:
        ring = ((row // (2 * size)) == (col // (2 * size))) & ((row // size) != (col // size))
        right = {
            p: mul(jnp.where(ring, lowers[p], jnp.zeros((), BF16)), inverses[p]) for p in problems
        }
        for p in problems:
            inverses[p] = inverses[p] - mul(inverses[p], right[p])
        size = 2 * size
    eye = lax.broadcasted_iota(jnp.int32, (width, width), 0) == lax.broadcasted_iota(
        jnp.int32, (width, width), 1
    )
    for h in range(heads):
        cut = slice(h * width, (h + 1) * width)
        own_sum = None
        reads = []
        for d in range(2):
            p = (h, d)
            written, read_own, q_b = products[p]
            a_full, q_full, b_tail, c_tail = [side[:, cut] for side in sides[d][4:]]
            solved = mul(inverses[p], jnp.concatenate([written, a_full], axis=1))
            back = mul(q_b, solved)
            own = read_own - back[:, :width]
            gain = q_full - back[:, width:]
            order = range(chunks - 1, -1, -1) if d else range(chunks)
            carry = None
            owns, gains = [None] * chunks, [None] * chunks
            for c in order:
                part = slice(c * chunk, (c + 1) * chunk)
                joint = mul(solved[part], b_tail[part], 0, 0)
                decayed = jnp.exp(ends[c][:, cut])
                step_p = jnp.where(eye, decayed, 0.0) - joint[width:]
                step_q = mul(values[part, cut], c_tail[part], 0, 0) - joint[:width]
                if carry is None:
                    owns[c], gains[c] = own[part], gain[part]
                    carry = jnp.concatenate([step_p, step_q], axis=0)
                else:
                    moved = mul(gain[part], carry, 1, 1)
                    gains[c] = moved[:, :width]
                    owns[c] = own[part] + moved[:, width:]
                    carry = mul(carry, step_p)
                    carry = jnp.concatenate([carry[:width], carry[width:] + step_q], axis=0)
            totals_ref[d, h] = jnp.concatenate([carry[:width], carry[width:]], axis=1).astype(BF16)
            reads.append(jnp.concatenate(gains, axis=0))
            own_whole = jnp.concatenate(owns, axis=0)
            own_sum = own_whole if own_sum is None else own_sum + own_whole
        read_ref[:, 2 * h * width : 2 * (h + 1) * width] = jnp.concatenate(reads, axis=1).astype(
            BF16
        )
        own_ref[:, cut] = own_sum


def finish_kernel(heads, width, where_ref, totals_ref, read_ref, own_ref, gain_ref, out_ref, res):
    me = where_ref[0]
    count = totals_ref.shape[0]
    states = {(d, h): jnp.zeros((width, width), F32) for d in range(2) for h in range(heads)}
    for j in range(count):
        for d in range(2):
            owner = count - 1 - j if d else j
            active = (owner > me) if d else (owner < me)
            for h in range(heads):
                both = totals_ref[owner, d, h]
                fresh = mul(states[d, h], both[:, :width]) + both[:, width:].astype(F32)
                states[d, h] = jnp.where(active, fresh, states[d, h])
    parts = []
    for h in range(heads):
        cut = slice(h * width, (h + 1) * width)
        pair = jnp.concatenate([states[0, h], states[1, h]], axis=1)
        mixed = own_ref[:, cut] + mul(
            read_ref[:, 2 * h * width : 2 * (h + 1) * width], pair, 1, 1
        )
        centre = mixed - jnp.mean(mixed, axis=-1, keepdims=True)
        parts.append(
            centre * lax.rsqrt(jnp.mean(centre * centre, axis=-1, keepdims=True) + 1e-05)
        )
    grouped = (jnp.concatenate(parts, axis=1) * gain_ref[...]).astype(BF16)
    res[...] = jnp.dot(grouped, out_ref[...], preferred_element_type=F32).astype(BF16)


def local_pass(heads, width, *operands):
    tokens = operands[0].shape[0]
    return pl.pallas_call(
        functools.partial(local_kernel, heads, width),
        out_shape=(
            jax.ShapeDtypeStruct((2, heads, width, 2 * width), BF16),
            jax.ShapeDtypeStruct((tokens, 2 * heads * width), BF16),
            jax.ShapeDtypeStruct((tokens, heads * width), F32),
        ),
        in_specs=[pl.BlockSpec(memory_space=pltpu.VMEM)] * len(operands),
        out_specs=(pl.BlockSpec(memory_space=pltpu.VMEM),) * 3,
        cost_estimate=pl.CostEstimate(
            flops=2000000000, bytes_accessed=20000000, transcendentals=0
        ),
        name="mix_local",
    )(*operands)


def finish_pass(heads, width, where, totals, read, own, gain, w_output):
    return pl.pallas_call(
        functools.partial(finish_kernel, heads, width),
        out_shape=jax.ShapeDtypeStruct((own.shape[0], w_output.shape[1]), BF16),
        in_specs=[pl.BlockSpec(memory_space=pltpu.SMEM)]
        + [pl.BlockSpec(memory_space=pltpu.VMEM)] * 5,
        out_specs=pl.BlockSpec(memory_space=pltpu.VMEM),
        cost_estimate=pl.CostEstimate(
            flops=1000000000, bytes_accessed=10000000, transcendentals=0
        ),
        name="mix_finish",
    )(where, totals, read, own, gain, w_output)


def route_tables(route_rows, weight_rows, expert_count, slot_count):
    route_list = route_rows.reshape(-1)
    onehot = (route_list[:, None] == jnp.arange(expert_count, dtype=jnp.int32)[None, :]).astype(
        jnp.int32
    )
    slot_index = jnp.sum((jnp.cumsum(onehot, axis=0) - onehot) * onehot, axis=1)
    target = (route_list * slot_count + slot_index).reshape(route_rows.shape)
    columns = jnp.arange(expert_count * slot_count, dtype=jnp.int32)
    matches = target[:, :, None] == columns[None, None, :]
    placing = jnp.sum(matches.astype(jnp.int32), axis=1).astype(jnp.bfloat16)
    rounded = weight_rows.astype(jnp.bfloat16)
    weighing = jnp.sum(jnp.where(matches, rounded[:, :, None], jnp.zeros((), jnp.bfloat16)), axis=1)
    return (placing, weighing)


def expert_hidden(slot_rows, gate_shard, up_shard):
    flattened = slot_rows.reshape(-1, slot_rows.shape[-1])
    gate_part = jnp.dot(flattened, gate_shard, preferred_element_type=jnp.float32)
    up_part = jnp.dot(flattened, up_shard, preferred_element_type=jnp.float32)
    hidden = (jax.nn.silu(gate_part) * up_part).astype(jnp.bfloat16)
    return hidden.reshape(slot_rows.shape[:-1] + (gate_shard.shape[1],))


def shards(
    mixer_input_rows,
    mix_gain,
    w_recept,
    w_key,
    w_value,
    lowered_map_factor,
    decay_up,
    rate_up,
    decay_base,
    rate_base,
    decay_shift,
    out_gain,
    w_output,
    moe_rows,
    moe_gain,
    routes,
    route_weight,
    exp_gate,
    exp_up,
    exp_down,
):
    head_count = decay_shift.shape[1]
    head_width = w_recept.shape[1] // head_count
    totals, read, own = local_pass(
        head_count,
        head_width,
        mixer_input_rows,
        mix_gain[None],
        w_recept,
        w_key,
        w_value,
        lowered_map_factor,
        decay_up,
        rate_up,
        decay_base[None],
        rate_base[None],
        decay_shift,
    )
    gathered = lax.all_gather(totals[None], "ep", axis=0, tiled=True)
    where = lax.axis_index("ep").astype(jnp.int32)[None]
    partial_mix = finish_pass(
        head_count, head_width, where, gathered, read, own, out_gain[None], w_output
    )
    mix_out = lax.psum_scatter(partial_mix, "tp", scatter_dimension=0, tiled=True)
    group_rows = moe_rows.shape[0]
    experts = lax.axis_size("ep")
    slots = 4 * group_rows // experts
    moe_normed = row_norm(moe_rows, moe_gain)
    placing, weighing = route_tables(routes, route_weight, experts, slots)
    buffer = lax.dot_general(
        placing, moe_normed, (((0,), (0,)), ((), ())), preferred_element_type=jnp.float32
    )
    buffer = buffer.astype(jnp.bfloat16).reshape(experts, slots, -1)
    gate_shard = exp_gate[0]
    up_shard = exp_up[0]
    down_shard = exp_down[0]
    arrived = lax.all_to_all(buffer, "ep", split_axis=0, concat_axis=0, tiled=True)
    hidden = expert_hidden(arrived, gate_shard, up_shard)
    partial_sum = jnp.dot(
        hidden.reshape(-1, hidden.shape[-1]), down_shard, preferred_element_type=jnp.float32
    )
    partial_sum = partial_sum.reshape(experts, slots, -1)
    summed = lax.psum_scatter(
        partial_sum.astype(jnp.bfloat16), "tp", scatter_dimension=2, tiled=True
    )
    returned = lax.all_to_all(summed, "ep", split_axis=0, concat_axis=0, tiled=True)
    moe_out = jnp.dot(
        weighing, returned.reshape(experts * slots, -1), preferred_element_type=jnp.float32
    )
    return (mix_out, moe_out.astype(jnp.bfloat16))


def solution(mesh):
    return jax.shard_map(
        shards,
        mesh=mesh,
        in_specs=(
            P("ep", None),
            P(),
            P(None, "tp"),
            P(None, "tp"),
            P(None, "tp"),
            P(),
            P(None, "tp"),
            P(None, "tp"),
            P("tp"),
            P("tp"),
            P("ep", "tp"),
            P("tp"),
            P("tp", None),
            P("ep", None),
            P(),
            P("ep", None),
            P("ep", None),
            P("ep", None, "tp"),
            P("ep", None, "tp"),
            P("ep", "tp", None),
        ),
        out_specs=(P(("ep", "tp"), None), P("ep", "tp")),
        check_vma=False,
    )
```

```python
import functools
import math

import jax
import jax.numpy as jnp
from jax import lax
from jax.experimental import pallas as pl
from jax.experimental.pallas import tpu as pltpu
from jax.sharding import PartitionSpec as P

HIGHEST = lax.Precision.HIGHEST
DECAY_SCALE = math.exp(-0.5)


def row_norm(row_block, gain_vector):
    entries = row_block.astype(jnp.float32)
    factor = lax.rsqrt(jnp.mean(entries * entries, axis=-1, keepdims=True) + 1e-06)
    return (entries * factor * gain_vector).astype(jnp.bfloat16)


F32 = jnp.float32
BF16 = jnp.bfloat16
CHUNK = 64


def mul(left, right, left_dim=1, right_dim=0):
    return lax.dot_general(
        left.astype(BF16),
        right.astype(BF16),
        (((left_dim,), (right_dim,)), ((), ())),
        preferred_element_type=F32,
    )


def local_kernel(
    heads,
    width,
    rows_ref,
    gain_ref,
    recept_ref,
    key_ref,
    value_ref,
    low_ref,
    decay_up_ref,
    rate_up_ref,
    decay_base_ref,
    rate_base_ref,
    shift_ref,
    totals_ref,
    read_ref,
    own_ref,
):
    tokens = rows_ref.shape[0]
    chunk = min(CHUNK, tokens)
    chunks = tokens // chunk
    normed = row_norm(rows_ref[...], gain_ref[...])
    recept = jnp.dot(normed, recept_ref[...], preferred_element_type=F32).astype(BF16)
    keys = jnp.dot(normed, key_ref[...], preferred_element_type=F32).astype(BF16).astype(F32)
    values = jnp.dot(normed, value_ref[...], preferred_element_type=F32).astype(BF16)
    recept = recept.astype(F32)
    low = jnp.tanh(jnp.dot(normed, low_ref[...], preferred_element_type=F32)).astype(BF16)
    decay_pre = decay_base_ref[...] + jnp.dot(low, decay_up_ref[...], preferred_element_type=F32)
    rate = jax.nn.sigmoid(
        rate_base_ref[...] + jnp.dot(low, rate_up_ref[...], preferred_element_type=F32)
    )
    shift = shift_ref[...]
    shift_wide = jnp.concatenate(
        [jnp.broadcast_to(shift[:, h : h + 1], (tokens, width)) for h in range(heads)], axis=1
    )
    log_decay = -DECAY_SCALE * jax.nn.sigmoid(decay_pre) + shift_wide

    row = lax.broadcasted_iota(jnp.int32, (tokens, tokens), 0)
    col = lax.broadcasted_iota(jnp.int32, (tokens, tokens), 1)
    same = (row // chunk) == (col // chunk)
    lower = jnp.where(same & (row >= col), 1.0, 0.0).astype(F32)
    running = jnp.dot(lower, log_decay, precision=HIGHEST, preferred_element_type=F32)
    ends = [running[(c + 1) * chunk - 1 : (c + 1) * chunk, :] for c in range(chunks)]
    total = jnp.concatenate(
        [jnp.broadcast_to(end, (chunk, end.shape[1])) for end in ends], axis=0
    )
    half = 0.5 * total
    squares = keys * keys
    unit = jnp.concatenate(
        [
            keys[:, h * width : (h + 1) * width]
            * lax.rsqrt(
                jnp.sum(squares[:, h * width : (h + 1) * width], axis=-1, keepdims=True) + 1e-06
            )
            for h in range(heads)
        ],
        axis=1,
    )
    learned = unit * rate
    sides = []
    for reverse in (False, True):
        upto = total - running + log_decay if reverse else running
        before = upto - log_decay
        up_scale = jnp.exp(upto - half)
        down_scale = jnp.exp(half - upto)
        tail = jnp.exp(total - upto)
        sides.append(
            (
                (unit * jnp.exp(before - half)).astype(BF16),
                (recept * up_scale).astype(BF16),
                (learned * down_scale).astype(BF16),
                (keys * down_scale).astype(BF16),
                unit * jnp.exp(before),
                recept * jnp.exp(upto),
                (learned * tail).astype(BF16),
                (keys * tail).astype(BF16),
            )
        )
    problems = [(h, d) for h in range(heads) for d in range(2)]
    products, inverses, lowers = {}, {}, {}
    for p in problems:
        h, d = p
        cut = slice(h * width, (h + 1) * width)
        a_side, q_side, b_side, c_side = [side[:, cut] for side in sides[d][:4]]
        pair = mul(
            jnp.concatenate([a_side, q_side], axis=0),
            jnp.concatenate([b_side, c_side], axis=0),
            1,
            1,
        )
        strict = same & ((row < col) if d else (row > col))
        whole = same & ((row <= col) if d else (row >= col))
        a_b = jnp.where(strict, pair[:tokens, :tokens], 0.0)
        a_c = jnp.where(strict, pair[:tokens, tokens:], 0.0)
        q_b = jnp.where(whole, pair[tokens:, :tokens], 0.0)
        q_c = jnp.where(whole, pair[tokens:, tokens:], 0.0)
        by_value = mul(jnp.concatenate([a_c, q_c], axis=0), values[:, cut])
        products[p] = (by_value[:tokens], by_value[tokens:], q_b)
        lowers[p] = a_b.astype(BF16)
        near = (row // 2) == (col // 2)
        inverses[p] = jnp.where(row == col, 1.0, jnp.where(near, -a_b, 0.0))
    size = 2
    while size < chunk:
        ring = ((row // (2 * size)) == (col // (2 * size))) & ((row // size) != (col // size))
        right = {
            p: mul(jnp.where(ring, lowers[p], jnp.zeros((), BF16)), inverses[p]) for p in problems
        }
        for p in problems:
            inverses[p] = inverses[p] - mul(inverses[p], right[p])
        size = 2 * size
    eye = lax.broadcasted_iota(jnp.int32, (width, width), 0) == lax.broadcasted_iota(
        jnp.int32, (width, width), 1
    )
    for h in range(heads):
        cut = slice(h * width, (h + 1) * width)
        own_sum = None
        reads = []
        for d in range(2):
            p = (h, d)
            written, read_own, q_b = products[p]
            a_full, q_full, b_tail, c_tail = [side[:, cut] for side in sides[d][4:]]
            solved = mul(inverses[p], jnp.concatenate([written, a_full], axis=1))
            back = mul(q_b, solved)
            own = read_own - back[:, :width]
            gain = q_full - back[:, width:]
            order = range(chunks - 1, -1, -1) if d else range(chunks)
            carry = None
            owns, gains = [None] * chunks, [None] * chunks
            for c in order:
                part = slice(c * chunk, (c + 1) * chunk)
                joint = mul(solved[part], b_tail[part], 0, 0)
                decayed = jnp.exp(ends[c][:, cut])
                step_p = jnp.where(eye, decayed, 0.0) - joint[width:]
                step_q = mul(values[part, cut], c_tail[part], 0, 0) - joint[:width]
                if carry is None:
                    owns[c], gains[c] = own[part], gain[part]
                    carry = jnp.concatenate([step_p, step_q], axis=0)
                else:
                    moved = mul(gain[part], carry, 1, 1)
                    gains[c] = moved[:, :width]
                    owns[c] = own[part] + moved[:, width:]
                    carry = mul(carry, step_p)
                    carry = jnp.concatenate([carry[:width], carry[width:] + step_q], axis=0)
            totals_ref[d, h] = jnp.concatenate([carry[:width], carry[width:]], axis=1).astype(BF16)
            reads.append(jnp.concatenate(gains, axis=0))
            own_whole = jnp.concatenate(owns, axis=0)
            own_sum = own_whole if own_sum is None else own_sum + own_whole
        read_ref[:, 2 * h * width : 2 * (h + 1) * width] = jnp.concatenate(reads, axis=1).astype(
            BF16
        )
        own_ref[:, cut] = own_sum


def finish_kernel(heads, width, where_ref, totals_ref, read_ref, own_ref, gain_ref, out_ref, res):
    me = where_ref[0]
    count = totals_ref.shape[0]
    states = {(d, h): jnp.zeros((width, width), F32) for d in range(2) for h in range(heads)}
    for j in range(count):
        for d in range(2):
            owner = count - 1 - j if d else j
            active = (owner > me) if d else (owner < me)
            for h in range(heads):
                both = totals_ref[owner, h]
                fresh = mul(states[d, h], both[:, :width]) + both[:, width:].astype(F32)
                states[d, h] = jnp.where(active, fresh, states[d, h])
    parts = []
    for h in range(heads):
        cut = slice(h * width, (h + 1) * width)
        pair = jnp.concatenate([states[0, h], states[1, h]], axis=1)
        mixed = own_ref[:, cut] + mul(
            read_ref[:, 2 * h * width : 2 * (h + 1) * width], pair, 1, 1
        )
        centre = mixed - jnp.mean(mixed, axis=-1, keepdims=True)
        parts.append(
            centre * lax.rsqrt(jnp.mean(centre * centre, axis=-1, keepdims=True) + 1e-05)
        )
    grouped = (jnp.concatenate(parts, axis=1) * gain_ref[...]).astype(BF16)
    res[...] = jnp.dot(grouped, out_ref[...], preferred_element_type=F32).astype(BF16)


def local_pass(heads, width, *operands):
    tokens = operands[0].shape[0]
    return pl.pallas_call(
        functools.partial(local_kernel, heads, width),
        out_shape=(
            jax.ShapeDtypeStruct((2, heads, width, 2 * width), BF16),
            jax.ShapeDtypeStruct((tokens, 2 * heads * width), BF16),
            jax.ShapeDtypeStruct((tokens, heads * width), F32),
        ),
        in_specs=[pl.BlockSpec(memory_space=pltpu.VMEM)] * len(operands),
        out_specs=(pl.BlockSpec(memory_space=pltpu.VMEM),) * 3,
        cost_estimate=pl.CostEstimate(
            flops=2000000000, bytes_accessed=20000000, transcendentals=0
        ),
        name="mix_local",
    )(*operands)


def finish_pass(heads, width, where, totals, read, own, gain, w_output):
    return pl.pallas_call(
        functools.partial(finish_kernel, heads, width),
        out_shape=jax.ShapeDtypeStruct((own.shape[0], w_output.shape[1]), BF16),
        in_specs=[pl.BlockSpec(memory_space=pltpu.SMEM)]
        + [pl.BlockSpec(memory_space=pltpu.VMEM)] * 5,
        out_specs=pl.BlockSpec(memory_space=pltpu.VMEM),
        cost_estimate=pl.CostEstimate(
            flops=1000000000, bytes_accessed=10000000, transcendentals=0
        ),
        name="mix_finish",
    )(where, totals, read, own, gain, w_output)


MESH_ID = pl.DeviceIdType.MESH


def greet(ep_count, tp_count):
    me, lane = lax.axis_index("ep"), lax.axis_index("tp")
    barrier = pltpu.get_barrier_semaphore()
    for k in range(1, ep_count):
        pl.semaphore_signal(
            barrier, inc=1, device_id=(lax.rem(me + k, ep_count), lane), device_id_type=MESH_ID
        )
    for k in range(1, tp_count):
        pl.semaphore_signal(
            barrier, inc=1, device_id=(me, lax.rem(lane + k, tp_count)), device_id_type=MESH_ID
        )
    pl.semaphore_wait(barrier, ep_count + tp_count - 2)


def remote(source, target, send_sem, recv_sem, device):
    return pltpu.make_async_remote_copy(
        src_ref=source,
        dst_ref=target,
        send_sem=send_sem,
        recv_sem=recv_sem,
        device_id=device,
        device_id_type=MESH_ID,
    )


def dispatch_kernel(
    ep_count,
    tp_count,
    buffer_ref,
    totals_ref,
    arrived_ref,
    gathered_ref,
    ep_send,
    ep_recv,
    row_send,
    row_recv,
    pair_send,
    pair_recv,
    total_send,
    total_recv,
    keep_sem,
):
    me, lane = lax.axis_index("ep"), lax.axis_index("tp")
    width = buffer_ref.shape[2] // tp_count
    rows = tp_count // 2
    mate = lane + 1 - 2 * lax.rem(lane, 2)
    greet(ep_count, tp_count)

    def columns(of):
        return pl.ds(pl.multiple_of(of * width, width), width)

    first, second, third, sums = [], [], [], []
    for k in range(1, ep_count):
        peer = lax.rem(me + k, ep_count)
        copy = remote(
            buffer_ref.at[peer, :, columns(lane)],
            arrived_ref.at[me, :, columns(lane)],
            ep_send.at[k],
            ep_recv.at[k],
            (peer, lane),
        )
        copy.start()
        first.append(copy)
    for k in range(1, ep_count):
        peer = lax.rem(me + k, ep_count)
        direction = jnp.where(peer > me, 0, 1)
        copy = remote(
            totals_ref.at[direction],
            gathered_ref.at[me],
            total_send.at[k],
            total_recv.at[k],
            (peer, lane),
        )
        copy.start()
        sums.append(copy)
    keep = pltpu.make_async_copy(buffer_ref.at[me], arrived_ref.at[me], keep_sem.at[0])
    keep.start()
    keep_total = pltpu.make_async_copy(totals_ref.at[0], gathered_ref.at[me], keep_sem.at[1])
    keep_total.start()
    for k in range(1, ep_count):
        owner = lax.rem(me + ep_count - k, ep_count)
        first[k - 1].wait_recv()
        block = arrived_ref.at[owner, :, columns(lane)]
        for j in range(1, rows):
            copy = remote(
                block,
                block,
                row_send.at[j, k],
                row_recv.at[j, k],
                (me, lax.rem(lane + 2 * j, tp_count)),
            )
            copy.start()
            second.append((j, owner, k, copy))
        copy = remote(block, block, pair_send.at[0, k], pair_recv.at[0, k], (me, mate))
        copy.start()
        third.append(copy)
    for j, owner, k, copy in second:
        copy.wait_recv()
        block = arrived_ref.at[owner, :, columns(lax.rem(lane + tp_count - 2 * j, tp_count))]
        passed = remote(block, block, pair_send.at[j, k], pair_recv.at[j, k], (me, mate))
        passed.start()
        third.append(passed)
    for copy in third:
        copy.wait_recv()
    for copy in sums:
        copy.wait_recv()
    for copy in first + [item[3] for item in second] + third + sums:
        copy.wait_send()
    keep.wait()
    keep_total.wait()


def dispatch_pass(ep_count, tp_count, buffer, totals):
    rows = tp_count // 2
    dma = pltpu.SemaphoreType.DMA
    return pl.pallas_call(
        functools.partial(dispatch_kernel, ep_count, tp_count),
        out_shape=(
            jax.ShapeDtypeStruct(buffer.shape, BF16),
            jax.ShapeDtypeStruct((ep_count,) + totals.shape[1:], BF16),
        ),
        in_specs=[pl.BlockSpec(memory_space=pltpu.VMEM)] * 2,
        out_specs=(pl.BlockSpec(memory_space=pltpu.VMEM),) * 2,
        scratch_shapes=[
            dma((ep_count,)),
            dma((ep_count,)),
            dma((rows, ep_count)),
            dma((rows, ep_count)),
            dma((rows, ep_count)),
            dma((rows, ep_count)),
            dma((ep_count,)),
            dma((ep_count,)),
            dma((2,)),
        ],
        compiler_params=pltpu.CompilerParams(collective_id=1, has_side_effects=True),
        name="dispatch",
    )(buffer, totals)


def return_kernel(
    ep_count,
    tp_count,
    partial_ref,
    mix_ref,
    back_ref,
    mix_out_ref,
    pair_in,
    pair_sum,
    row_in,
    result,
    mix_in,
    pair_send,
    pair_recv,
    row_send,
    row_recv,
    ep_send,
    ep_recv,
    mix_send,
    mix_recv,
):
    me, lane = lax.axis_index("ep"), lax.axis_index("tp")
    width = partial_ref.shape[2] // tp_count
    rows = tp_count // 2
    core = lax.rem(lane, 2)
    mine = lane // 2
    mate = lane + 1 - 2 * core
    mix_rows = mix_out_ref.shape[0]
    greet(ep_count, tp_count)

    def columns(of):
        return pl.ds(pl.multiple_of(of * width, width), width)

    groups = [lax.rem(me + k, ep_count) for k in range(1, ep_count + 1)]
    first = []
    for k, group in enumerate(groups):
        for j in range(rows):
            copy = remote(
                partial_ref.at[group, :, columns(2 * j + 1 - core)],
                pair_in.at[k, j],
                pair_send.at[k, j],
                pair_recv.at[k, j],
                (me, mate),
            )
            copy.start()
            first.append(copy)
    second = []
    for k, group in enumerate(groups):
        for j in range(rows):
            first[k * rows + j].wait_recv()
        for j in range(rows):
            target = lax.rem(mine + j, rows)
            pair_sum[k, j] = (
                partial_ref[group, :, columns(2 * target + core)].astype(F32)
                + pair_in[k, target].astype(F32)
            ).astype(BF16)
            if j > 0:
                copy = remote(
                    pair_sum.at[k, j],
                    row_in.at[k, j],
                    row_send.at[k, j],
                    row_recv.at[k, j],
                    (me, 2 * target + core),
                )
                copy.start()
                second.append(copy)
    mixes = []
    for j in range(1, tp_count):
        peer = lax.rem(lane + j, tp_count)
        copy = remote(
            mix_ref.at[pl.ds(pl.multiple_of(peer * mix_rows, mix_rows), mix_rows)],
            mix_in.at[j],
            mix_send.at[j],
            mix_recv.at[j],
            (me, peer),
        )
        copy.start()
        mixes.append(copy)
    third = []
    for k, group in enumerate(groups):
        total = pair_sum[k, 0].astype(F32)
        for j in range(1, rows):
            second[k * (rows - 1) + j - 1].wait_recv()
            total = total + row_in[k, j].astype(F32)
        if k < ep_count - 1:
            result[k] = total.astype(BF16)
            copy = remote(
                result.at[k], back_ref.at[me], ep_send.at[k], ep_recv.at[k], (group, lane)
            )
            copy.start()
            third.append(copy)
        else:
            back_ref[me] = total.astype(BF16)
    own = mix_ref[pl.ds(pl.multiple_of(lane * mix_rows, mix_rows), mix_rows), :].astype(F32)
    for j in range(1, tp_count):
        mixes[j - 1].wait_recv()
        own = own + mix_in[j].astype(F32)
    mix_out_ref[...] = own.astype(BF16)
    for copy in third:
        copy.wait_recv()
    for copy in first + second + mixes + third:
        copy.wait_send()


def return_pass(ep_count, tp_count, partial_sum, partial_mix):
    rows = tp_count // 2
    dma = pltpu.SemaphoreType.DMA
    slots, features = partial_sum.shape[1:]
    width = features // tp_count
    mix_rows = partial_mix.shape[0] // tp_count
    return pl.pallas_call(
        functools.partial(return_kernel, ep_count, tp_count),
        out_shape=(
            jax.ShapeDtypeStruct((ep_count, slots, width), BF16),
            jax.ShapeDtypeStruct((mix_rows, features), BF16),
        ),
        in_specs=[pl.BlockSpec(memory_space=pltpu.VMEM)] * 2,
        out_specs=(pl.BlockSpec(memory_space=pltpu.VMEM),) * 2,
        scratch_shapes=[
            pltpu.VMEM((ep_count, rows, slots, width), BF16),
            pltpu.VMEM((ep_count, rows, slots, width), BF16),
            pltpu.VMEM((ep_count, rows, slots, width), BF16),
            pltpu.VMEM((ep_count, slots, width), BF16),
            pltpu.VMEM((tp_count, mix_rows, features), BF16),
            dma((ep_count, rows)),
            dma((ep_count, rows)),
            dma((ep_count, rows)),
            dma((ep_count, rows)),
            dma((ep_count,)),
            dma((ep_count,)),
            dma((tp_count,)),
            dma((tp_count,)),
        ],
        compiler_params=pltpu.CompilerParams(collective_id=2, has_side_effects=True),
        name="return",
    )(partial_sum, partial_mix)


def route_tables(route_rows, weight_rows, expert_count, slot_count):
    route_list = route_rows.reshape(-1)
    onehot = (route_list[:, None] == jnp.arange(expert_count, dtype=jnp.int32)[None, :]).astype(
        jnp.int32
    )
    slot_index = jnp.sum((jnp.cumsum(onehot, axis=0) - onehot) * onehot, axis=1)
    target = (route_list * slot_count + slot_index).reshape(route_rows.shape)
    columns = jnp.arange(expert_count * slot_count, dtype=jnp.int32)
    matches = target[:, :, None] == columns[None, None, :]
    placing = jnp.sum(matches.astype(jnp.int32), axis=1).astype(jnp.bfloat16)
    rounded = weight_rows.astype(jnp.bfloat16)
    weighing = jnp.sum(jnp.where(matches, rounded[:, :, None], jnp.zeros((), jnp.bfloat16)), axis=1)
    return (placing, weighing)


def expert_hidden(slot_rows, gate_shard, up_shard):
    flattened = slot_rows.reshape(-1, slot_rows.shape[-1])
    gate_part = jnp.dot(flattened, gate_shard, preferred_element_type=jnp.float32)
    up_part = jnp.dot(flattened, up_shard, preferred_element_type=jnp.float32)
    hidden = (jax.nn.silu(gate_part) * up_part).astype(jnp.bfloat16)
    return hidden.reshape(slot_rows.shape[:-1] + (gate_shard.shape[1],))


def shards(
    mixer_input_rows,
    mix_gain,
    w_recept,
    w_key,
    w_value,
    lowered_map_factor,
    decay_up,
    rate_up,
    decay_base,
    rate_base,
    decay_shift,
    out_gain,
    w_output,
    moe_rows,
    moe_gain,
    routes,
    route_weight,
    exp_gate,
    exp_up,
    exp_down,
):
    head_count = decay_shift.shape[1]
    head_width = w_recept.shape[1] // head_count
    totals, read, own = local_pass(
        head_count,
        head_width,
        mixer_input_rows,
        mix_gain[None],
        w_recept,
        w_key,
        w_value,
        lowered_map_factor,
        decay_up,
        rate_up,
        decay_base[None],
        rate_base[None],
        decay_shift,
    )
    group_rows = moe_rows.shape[0]
    experts = lax.axis_size("ep")
    slots = 4 * group_rows // experts
    moe_normed = row_norm(moe_rows, moe_gain)
    placing, weighing = route_tables(routes, route_weight, experts, slots)
    buffer = lax.dot_general(
        placing, moe_normed, (((0,), (0,)), ((), ())), preferred_element_type=jnp.float32
    )
    buffer = buffer.astype(jnp.bfloat16).reshape(experts, slots, -1)
    gate_shard = exp_gate[0]
    up_shard = exp_up[0]
    down_shard = exp_down[0]
    lanes = lax.axis_size("tp")
    small = experts <= 8 and lanes == 4
    if small:
        arrived, gathered = dispatch_pass(experts, lanes, buffer, totals)
    else:
        arrived = lax.all_to_all(buffer, "ep", split_axis=0, concat_axis=0, tiled=True)
        both = lax.all_gather(totals[None], "ep", axis=0, tiled=True)
        owners = jnp.arange(experts)[:, None, None, None]
        gathered = jnp.where(owners < lax.axis_index("ep"), both[:, 0], both[:, 1])
    where = lax.axis_index("ep").astype(jnp.int32)[None]
    partial_mix = finish_pass(
        head_count, head_width, where, gathered, read, own, out_gain[None], w_output
    )
    hidden = expert_hidden(arrived, gate_shard, up_shard)
    partial_sum = jnp.dot(
        hidden.reshape(-1, hidden.shape[-1]), down_shard, preferred_element_type=jnp.float32
    )
    partial_sum = partial_sum.reshape(experts, slots, -1).astype(jnp.bfloat16)
    if small:
        returned, mix_out = return_pass(experts, lanes, partial_sum, partial_mix)
    else:
        mix_out = lax.psum_scatter(partial_mix, "tp", scatter_dimension=0, tiled=True)
        summed = lax.psum_scatter(partial_sum, "tp", scatter_dimension=2, tiled=True)
        returned = lax.all_to_all(summed, "ep", split_axis=0, concat_axis=0, tiled=True)
    moe_out = jnp.dot(
        weighing, returned.reshape(experts * slots, -1), preferred_element_type=jnp.float32
    )
    return (mix_out, moe_out.astype(jnp.bfloat16))


def solution(mesh):
    return jax.shard_map(
        shards,
        mesh=mesh,
        in_specs=(
            P("ep", None),
            P(),
            P(None, "tp"),
            P(None, "tp"),
            P(None, "tp"),
            P(),
            P(None, "tp"),
            P(None, "tp"),
            P("tp"),
            P("tp"),
            P("ep", "tp"),
            P("tp"),
            P("tp", None),
            P("ep", None),
            P(),
            P("ep", None),
            P("ep", None),
            P("ep", None, "tp"),
            P("ep", None, "tp"),
            P("ep", "tp", None),
        ),
        out_specs=(P(("ep", "tp"), None), P("ep", "tp")),
        check_vma=False,
    )
```

```python
import functools
import math

import jax
import jax.numpy as jnp
from jax import lax
from jax.experimental import pallas as pl
from jax.experimental.pallas import tpu as pltpu
from jax.sharding import PartitionSpec as P

HIGHEST = lax.Precision.HIGHEST
DECAY_SCALE = math.exp(-0.5)


def row_norm(row_block, gain_vector):
    entries = row_block.astype(jnp.float32)
    factor = lax.rsqrt(jnp.mean(entries * entries, axis=-1, keepdims=True) + 1e-06)
    return (entries * factor * gain_vector).astype(jnp.bfloat16)


F32 = jnp.float32
BF16 = jnp.bfloat16
CHUNK = 64


def mul(left, right, left_dim=1, right_dim=0):
    return lax.dot_general(
        left.astype(BF16),
        right.astype(BF16),
        (((left_dim,), (right_dim,)), ((), ())),
        preferred_element_type=F32,
    )


def local_kernel(
    heads,
    width,
    rows_ref,
    gain_ref,
    recept_ref,
    key_ref,
    value_ref,
    low_ref,
    decay_up_ref,
    rate_up_ref,
    decay_base_ref,
    rate_base_ref,
    shift_ref,
    totals_ref,
    read_ref,
    own_ref,
    midway=None,
):
    tokens = rows_ref.shape[0]
    chunk = min(CHUNK, tokens)
    chunks = tokens // chunk
    normed = row_norm(rows_ref[...], gain_ref[...])
    recept = jnp.dot(normed, recept_ref[...], preferred_element_type=F32).astype(BF16)
    keys = jnp.dot(normed, key_ref[...], preferred_element_type=F32).astype(BF16).astype(F32)
    values = jnp.dot(normed, value_ref[...], preferred_element_type=F32).astype(BF16)
    recept = recept.astype(F32)
    low = jnp.tanh(jnp.dot(normed, low_ref[...], preferred_element_type=F32)).astype(BF16)
    decay_pre = decay_base_ref[...] + jnp.dot(low, decay_up_ref[...], preferred_element_type=F32)
    rate = jax.nn.sigmoid(
        rate_base_ref[...] + jnp.dot(low, rate_up_ref[...], preferred_element_type=F32)
    )
    shift = shift_ref[...]
    shift_wide = jnp.concatenate(
        [jnp.broadcast_to(shift[:, h : h + 1], (tokens, width)) for h in range(heads)], axis=1
    )
    log_decay = -DECAY_SCALE * jax.nn.sigmoid(decay_pre) + shift_wide

    row = lax.broadcasted_iota(jnp.int32, (tokens, tokens), 0)
    col = lax.broadcasted_iota(jnp.int32, (tokens, tokens), 1)
    same = (row // chunk) == (col // chunk)
    lower = jnp.where(same & (row >= col), 1.0, 0.0).astype(F32)
    running = jnp.dot(lower, log_decay, precision=HIGHEST, preferred_element_type=F32)
    ends = [running[(c + 1) * chunk - 1 : (c + 1) * chunk, :] for c in range(chunks)]
    total = jnp.concatenate(
        [jnp.broadcast_to(end, (chunk, end.shape[1])) for end in ends], axis=0
    )
    half = 0.5 * total
    squares = keys * keys
    unit = jnp.concatenate(
        [
            keys[:, h * width : (h + 1) * width]
            * lax.rsqrt(
                jnp.sum(squares[:, h * width : (h + 1) * width], axis=-1, keepdims=True) + 1e-06
            )
            for h in range(heads)
        ],
        axis=1,
    )
    learned = unit * rate
    sides = []
    for reverse in (False, True):
        upto = total - running + log_decay if reverse else running
        before = upto - log_decay
        up_scale = jnp.exp(upto - half)
        down_scale = jnp.exp(half - upto)
        tail = jnp.exp(total - upto)
        sides.append(
            (
                (unit * jnp.exp(before - half)).astype(BF16),
                (recept * up_scale).astype(BF16),
                (learned * down_scale).astype(BF16),
                (keys * down_scale).astype(BF16),
                unit * jnp.exp(before),
                recept * jnp.exp(upto),
                (learned * tail).astype(BF16),
                (keys * tail).astype(BF16),
            )
        )
    problems = [(h, d) for h in range(heads) for d in range(2)]
    products, inverses, lowers = {}, {}, {}
    for p in problems:
        h, d = p
        cut = slice(h * width, (h + 1) * width)
        a_side, q_side, b_side, c_side = [side[:, cut] for side in sides[d][:4]]
        pair = mul(
            jnp.concatenate([a_side, q_side], axis=0),
            jnp.concatenate([b_side, c_side], axis=0),
            1,
            1,
        )
        strict = same & ((row < col) if d else (row > col))
        whole = same & ((row <= col) if d else (row >= col))
        a_b = jnp.where(strict, pair[:tokens, :tokens], 0.0)
        a_c = jnp.where(strict, pair[:tokens, tokens:], 0.0)
        q_b = jnp.where(whole, pair[tokens:, :tokens], 0.0)
        q_c = jnp.where(whole, pair[tokens:, tokens:], 0.0)
        by_value = mul(jnp.concatenate([a_c, q_c], axis=0), values[:, cut])
        products[p] = (by_value[:tokens], by_value[tokens:], q_b)
        lowers[p] = a_b.astype(BF16)
        near = (row // 2) == (col // 2)
        inverses[p] = jnp.where(row == col, 1.0, jnp.where(near, -a_b, 0.0))
    size = 2
    while size < chunk:
        ring = ((row // (2 * size)) == (col // (2 * size))) & ((row // size) != (col // size))
        right = {
            p: mul(jnp.where(ring, lowers[p], jnp.zeros((), BF16)), inverses[p]) for p in problems
        }
        for p in problems:
            inverses[p] = inverses[p] - mul(inverses[p], right[p])
        size = 2 * size
    if midway is not None:
        midway()
    eye = lax.broadcasted_iota(jnp.int32, (width, width), 0) == lax.broadcasted_iota(
        jnp.int32, (width, width), 1
    )
    for h in range(heads):
        cut = slice(h * width, (h + 1) * width)
        own_sum = None
        reads = []
        for d in range(2):
            p = (h, d)
            written, read_own, q_b = products[p]
            a_full, q_full, b_tail, c_tail = [side[:, cut] for side in sides[d][4:]]
            solved = mul(inverses[p], jnp.concatenate([written, a_full], axis=1))
            back = mul(q_b, solved)
            own = read_own - back[:, :width]
            gain = q_full - back[:, width:]
            order = range(chunks - 1, -1, -1) if d else range(chunks)
            carry = None
            owns, gains = [None] * chunks, [None] * chunks
            for c in order:
                part = slice(c * chunk, (c + 1) * chunk)
                joint = mul(solved[part], b_tail[part], 0, 0)
                decayed = jnp.exp(ends[c][:, cut])
                step_p = jnp.where(eye, decayed, 0.0) - joint[width:]
                step_q = mul(values[part, cut], c_tail[part], 0, 0) - joint[:width]
                if carry is None:
                    owns[c], gains[c] = own[part], gain[part]
                    carry = jnp.concatenate([step_p, step_q], axis=0)
                else:
                    moved = mul(gain[part], carry, 1, 1)
                    gains[c] = moved[:, :width]
                    owns[c] = own[part] + moved[:, width:]
                    carry = mul(carry, step_p)
                    carry = jnp.concatenate([carry[:width], carry[width:] + step_q], axis=0)
            totals_ref[d, h] = jnp.concatenate([carry[:width], carry[width:]], axis=1).astype(BF16)
            reads.append(jnp.concatenate(gains, axis=0))
            own_whole = jnp.concatenate(owns, axis=0)
            own_sum = own_whole if own_sum is None else own_sum + own_whole
        read_ref[:, 2 * h * width : 2 * (h + 1) * width] = jnp.concatenate(reads, axis=1).astype(
            BF16
        )
        own_ref[:, cut] = own_sum


def finish_kernel(heads, width, where_ref, *refs):
    finish_body(heads, width, where_ref[0], *refs)


def finish_body(heads, width, me, totals_ref, read_ref, own_ref, gain_ref, out_ref, res):
    count = totals_ref.shape[0]
    states = {(d, h): jnp.zeros((width, width), F32) for d in range(2) for h in range(heads)}
    for j in range(count):
        for d in range(2):
            owner = count - 1 - j if d else j
            active = (owner > me) if d else (owner < me)
            for h in range(heads):
                both = totals_ref[owner, h]
                fresh = mul(states[d, h], both[:, :width]) + both[:, width:].astype(F32)
                states[d, h] = jnp.where(active, fresh, states[d, h])
    parts = []
    for h in range(heads):
        cut = slice(h * width, (h + 1) * width)
        pair = jnp.concatenate([states[0, h], states[1, h]], axis=1)
        mixed = own_ref[:, cut] + mul(
            read_ref[:, 2 * h * width : 2 * (h + 1) * width], pair, 1, 1
        )
        centre = mixed - jnp.mean(mixed, axis=-1, keepdims=True)
        parts.append(
            centre * lax.rsqrt(jnp.mean(centre * centre, axis=-1, keepdims=True) + 1e-05)
        )
    grouped = (jnp.concatenate(parts, axis=1) * gain_ref[...]).astype(BF16)
    res[...] = jnp.dot(grouped, out_ref[...], preferred_element_type=F32).astype(BF16)


def local_pass(heads, width, *operands):
    tokens = operands[0].shape[0]
    return pl.pallas_call(
        functools.partial(local_kernel, heads, width),
        out_shape=(
            jax.ShapeDtypeStruct((2, heads, width, 2 * width), BF16),
            jax.ShapeDtypeStruct((tokens, 2 * heads * width), BF16),
            jax.ShapeDtypeStruct((tokens, heads * width), F32),
        ),
        in_specs=[pl.BlockSpec(memory_space=pltpu.VMEM)] * len(operands),
        out_specs=(pl.BlockSpec(memory_space=pltpu.VMEM),) * 3,
        cost_estimate=pl.CostEstimate(
            flops=2000000000, bytes_accessed=20000000, transcendentals=0
        ),
        name="mix_local",
    )(*operands)


def finish_pass(heads, width, where, totals, read, own, gain, w_output):
    return pl.pallas_call(
        functools.partial(finish_kernel, heads, width),
        out_shape=jax.ShapeDtypeStruct((own.shape[0], w_output.shape[1]), BF16),
        in_specs=[pl.BlockSpec(memory_space=pltpu.SMEM)]
        + [pl.BlockSpec(memory_space=pltpu.VMEM)] * 5,
        out_specs=pl.BlockSpec(memory_space=pltpu.VMEM),
        cost_estimate=pl.CostEstimate(
            flops=1000000000, bytes_accessed=10000000, transcendentals=0
        ),
        name="mix_finish",
    )(where, totals, read, own, gain, w_output)


MESH_ID = pl.DeviceIdType.MESH


def greet(ep_count, tp_count):
    me, lane = lax.axis_index("ep"), lax.axis_index("tp")
    barrier = pltpu.get_barrier_semaphore()
    for k in range(1, ep_count):
        pl.semaphore_signal(
            barrier, inc=1, device_id=(lax.rem(me + k, ep_count), lane), device_id_type=MESH_ID
        )
    for k in range(1, tp_count):
        pl.semaphore_signal(
            barrier, inc=1, device_id=(me, lax.rem(lane + k, tp_count)), device_id_type=MESH_ID
        )
    pl.semaphore_wait(barrier, ep_count + tp_count - 2)


def remote(source, target, send_sem, recv_sem, device):
    return pltpu.make_async_remote_copy(
        src_ref=source,
        dst_ref=target,
        send_sem=send_sem,
        recv_sem=recv_sem,
        device_id=device,
        device_id_type=MESH_ID,
    )


def dispatch_kernel(
    heads,
    head_width,
    ep_count,
    tp_count,
    buffer_ref,
    rows_ref,
    gain_ref,
    recept_ref,
    key_ref,
    value_ref,
    low_ref,
    decay_up_ref,
    rate_up_ref,
    decay_base_ref,
    rate_base_ref,
    shift_ref,
    arrived_ref,
    gathered_ref,
    read_ref,
    own_ref,
    totals_ref,
    ep_send,
    ep_recv,
    row_send,
    row_recv,
    pair_send,
    pair_recv,
    total_send,
    total_recv,
    keep_sem,
):
    me, lane = lax.axis_index("ep"), lax.axis_index("tp")
    width = buffer_ref.shape[2] // tp_count
    rows = tp_count // 2
    mate = lane + 1 - 2 * lax.rem(lane, 2)
    greet(ep_count, tp_count)

    def columns(of):
        return pl.ds(pl.multiple_of(of * width, width), width)

    first, second, third, sums = [], [], [], []
    for k in range(1, ep_count):
        peer = lax.rem(me + k, ep_count)
        copy = remote(
            buffer_ref.at[peer, :, columns(lane)],
            arrived_ref.at[me, :, columns(lane)],
            ep_send.at[k],
            ep_recv.at[k],
            (peer, lane),
        )
        copy.start()
        first.append(copy)
    keep = pltpu.make_async_copy(buffer_ref.at[me], arrived_ref.at[me], keep_sem.at[0])
    keep.start()

    def forward(k):
        owner = lax.rem(me + ep_count - k, ep_count)
        first[k - 1].wait_recv()
        block = arrived_ref.at[owner, :, columns(lane)]
        for j in range(1, rows):
            copy = remote(
                block,
                block,
                row_send.at[j, k],
                row_recv.at[j, k],
                (me, lax.rem(lane + 2 * j, tp_count)),
            )
            copy.start()
            second.append((j, owner, k, copy))
        copy = remote(block, block, pair_send.at[0, k], pair_recv.at[0, k], (me, mate))
        copy.start()
        third.append(copy)

    early = ep_count // 2

    def midway():
        for k in range(1, early):
            forward(k)

    local_kernel(
        heads,
        head_width,
        rows_ref,
        gain_ref,
        recept_ref,
        key_ref,
        value_ref,
        low_ref,
        decay_up_ref,
        rate_up_ref,
        decay_base_ref,
        rate_base_ref,
        shift_ref,
        totals_ref,
        read_ref,
        own_ref,
        midway,
    )
    for k in range(1, ep_count):
        peer = lax.rem(me + k, ep_count)
        direction = jnp.where(peer > me, 0, 1)
        copy = remote(
            totals_ref.at[direction],
            gathered_ref.at[me],
            total_send.at[k],
            total_recv.at[k],
            (peer, lane),
        )
        copy.start()
        sums.append(copy)
    keep_total = pltpu.make_async_copy(totals_ref.at[0], gathered_ref.at[me], keep_sem.at[1])
    keep_total.start()
    for k in range(early, ep_count):
        forward(k)
    for j, owner, k, copy in second:
        copy.wait_recv()
        block = arrived_ref.at[owner, :, columns(lax.rem(lane + tp_count - 2 * j, tp_count))]
        passed = remote(block, block, pair_send.at[j, k], pair_recv.at[j, k], (me, mate))
        passed.start()
        third.append(passed)
    for copy in third:
        copy.wait_recv()
    for copy in sums:
        copy.wait_recv()
    for copy in first + [item[3] for item in second] + third + sums:
        copy.wait_send()
    keep.wait()
    keep_total.wait()


def dispatch_pass(heads, head_width, ep_count, tp_count, buffer, *operands):
    tokens = operands[0].shape[0]
    rows = tp_count // 2
    dma = pltpu.SemaphoreType.DMA
    return pl.pallas_call(
        functools.partial(dispatch_kernel, heads, head_width, ep_count, tp_count),
        out_shape=(
            jax.ShapeDtypeStruct(buffer.shape, BF16),
            jax.ShapeDtypeStruct((ep_count, heads, head_width, 2 * head_width), BF16),
            jax.ShapeDtypeStruct((tokens, 2 * heads * head_width), BF16),
            jax.ShapeDtypeStruct((tokens, heads * head_width), F32),
        ),
        in_specs=[pl.BlockSpec(memory_space=pltpu.VMEM)] * (1 + len(operands)),
        out_specs=(pl.BlockSpec(memory_space=pltpu.VMEM),) * 4,
        scratch_shapes=[
            pltpu.VMEM((2, heads, head_width, 2 * head_width), BF16),
            dma((ep_count,)),
            dma((ep_count,)),
            dma((rows, ep_count)),
            dma((rows, ep_count)),
            dma((rows, ep_count)),
            dma((rows, ep_count)),
            dma((ep_count,)),
            dma((ep_count,)),
            dma((2,)),
        ],
        compiler_params=pltpu.CompilerParams(collective_id=1, has_side_effects=True),
        name="dispatch",
    )(buffer, *operands)


def return_kernel(
    heads,
    head_width,
    ep_count,
    tp_count,
    partial_ref,
    gathered_ref,
    read_ref,
    own_ref,
    gain_ref,
    out_ref,
    back_ref,
    mix_out_ref,
    mix_ref,
    pair_in,
    pair_sum,
    row_in,
    result,
    mix_in,
    pair_send,
    pair_recv,
    row_send,
    row_recv,
    ep_send,
    ep_recv,
    mix_send,
    mix_recv,
):
    me, lane = lax.axis_index("ep"), lax.axis_index("tp")
    width = partial_ref.shape[2] // tp_count
    rows = tp_count // 2
    core = lax.rem(lane, 2)
    mine = lane // 2
    mate = lane + 1 - 2 * core
    mix_rows = mix_out_ref.shape[0]
    greet(ep_count, tp_count)

    def columns(of):
        return pl.ds(pl.multiple_of(of * width, width), width)

    groups = [lax.rem(me + k, ep_count) for k in range(1, ep_count + 1)]
    first = []
    for k, group in enumerate(groups):
        for j in range(rows):
            copy = remote(
                partial_ref.at[group, :, columns(2 * j + 1 - core)],
                pair_in.at[k, j],
                pair_send.at[k, j],
                pair_recv.at[k, j],
                (me, mate),
            )
            copy.start()
            first.append(copy)
    second = []
    for k, group in enumerate(groups):
        for j in range(rows):
            first[k * rows + j].wait_recv()
        for j in range(rows):
            target = lax.rem(mine + j, rows)
            pair_sum[k, j] = (
                partial_ref[group, :, columns(2 * target + core)].astype(F32)
                + pair_in[k, target].astype(F32)
            ).astype(BF16)
            if j > 0:
                copy = remote(
                    pair_sum.at[k, j],
                    row_in.at[k, j],
                    row_send.at[k, j],
                    row_recv.at[k, j],
                    (me, 2 * target + core),
                )
                copy.start()
                second.append(copy)
    finish_body(
        heads, head_width, me, gathered_ref, read_ref, own_ref, gain_ref, out_ref, mix_ref
    )
    mixes = []
    for j in range(1, tp_count):
        peer = lax.rem(lane + j, tp_count)
        copy = remote(
            mix_ref.at[pl.ds(pl.multiple_of(peer * mix_rows, mix_rows), mix_rows)],
            mix_in.at[j],
            mix_send.at[j],
            mix_recv.at[j],
            (me, peer),
        )
        copy.start()
        mixes.append(copy)
    third = []
    for k, group in enumerate(groups):
        total = pair_sum[k, 0].astype(F32)
        for j in range(1, rows):
            second[k * (rows - 1) + j - 1].wait_recv()
            total = total + row_in[k, j].astype(F32)
        if k < ep_count - 1:
            result[k] = total.astype(BF16)
            copy = remote(
                result.at[k], back_ref.at[me], ep_send.at[k], ep_recv.at[k], (group, lane)
            )
            copy.start()
            third.append(copy)
        else:
            back_ref[me] = total.astype(BF16)
    own = mix_ref[pl.ds(pl.multiple_of(lane * mix_rows, mix_rows), mix_rows), :].astype(F32)
    for j in range(1, tp_count):
        mixes[j - 1].wait_recv()
        own = own + mix_in[j].astype(F32)
    mix_out_ref[...] = own.astype(BF16)
    for copy in third:
        copy.wait_recv()
    for copy in first + second + mixes + third:
        copy.wait_send()


def return_pass(heads, head_width, ep_count, tp_count, partial_sum, *operands):
    rows = tp_count // 2
    dma = pltpu.SemaphoreType.DMA
    slots, features = partial_sum.shape[1:]
    width = features // tp_count
    tokens = operands[1].shape[0]
    mix_rows = tokens // tp_count
    return pl.pallas_call(
        functools.partial(return_kernel, heads, head_width, ep_count, tp_count),
        out_shape=(
            jax.ShapeDtypeStruct((ep_count, slots, width), BF16),
            jax.ShapeDtypeStruct((mix_rows, features), BF16),
        ),
        in_specs=[pl.BlockSpec(memory_space=pltpu.VMEM)] * (1 + len(operands)),
        out_specs=(pl.BlockSpec(memory_space=pltpu.VMEM),) * 2,
        scratch_shapes=[
            pltpu.VMEM((tokens, features), BF16),
            pltpu.VMEM((ep_count, rows, slots, width), BF16),
            pltpu.VMEM((ep_count, rows, slots, width), BF16),
            pltpu.VMEM((ep_count, rows, slots, width), BF16),
            pltpu.VMEM((ep_count, slots, width), BF16),
            pltpu.VMEM((tp_count, mix_rows, features), BF16),
            dma((ep_count, rows)),
            dma((ep_count, rows)),
            dma((ep_count, rows)),
            dma((ep_count, rows)),
            dma((ep_count,)),
            dma((ep_count,)),
            dma((tp_count,)),
            dma((tp_count,)),
        ],
        compiler_params=pltpu.CompilerParams(collective_id=2, has_side_effects=True),
        name="return",
    )(partial_sum, *operands)


def route_tables(route_rows, weight_rows, expert_count, slot_count):
    route_list = route_rows.reshape(-1)
    onehot = (route_list[:, None] == jnp.arange(expert_count, dtype=jnp.int32)[None, :]).astype(
        jnp.int32
    )
    slot_index = jnp.sum((jnp.cumsum(onehot, axis=0) - onehot) * onehot, axis=1)
    target = (route_list * slot_count + slot_index).reshape(route_rows.shape)
    columns = jnp.arange(expert_count * slot_count, dtype=jnp.int32)
    matches = target[:, :, None] == columns[None, None, :]
    placing = jnp.sum(matches.astype(jnp.int32), axis=1).astype(jnp.bfloat16)
    rounded = weight_rows.astype(jnp.bfloat16)
    weighing = jnp.sum(jnp.where(matches, rounded[:, :, None], jnp.zeros((), jnp.bfloat16)), axis=1)
    return (placing, weighing)


def expert_hidden(slot_rows, gate_shard, up_shard):
    flattened = slot_rows.reshape(-1, slot_rows.shape[-1])
    gate_part = jnp.dot(flattened, gate_shard, preferred_element_type=jnp.float32)
    up_part = jnp.dot(flattened, up_shard, preferred_element_type=jnp.float32)
    hidden = (jax.nn.silu(gate_part) * up_part).astype(jnp.bfloat16)
    return hidden.reshape(slot_rows.shape[:-1] + (gate_shard.shape[1],))


def shards(
    mixer_input_rows,
    mix_gain,
    w_recept,
    w_key,
    w_value,
    lowered_map_factor,
    decay_up,
    rate_up,
    decay_base,
    rate_base,
    decay_shift,
    out_gain,
    w_output,
    moe_rows,
    moe_gain,
    routes,
    route_weight,
    exp_gate,
    exp_up,
    exp_down,
):
    head_count = decay_shift.shape[1]
    head_width = w_recept.shape[1] // head_count
    mix_operands = (
        mixer_input_rows,
        mix_gain[None],
        w_recept,
        w_key,
        w_value,
        lowered_map_factor,
        decay_up,
        rate_up,
        decay_base[None],
        rate_base[None],
        decay_shift,
    )
    group_rows = moe_rows.shape[0]
    experts = lax.axis_size("ep")
    slots = 4 * group_rows // experts
    moe_normed = row_norm(moe_rows, moe_gain)
    placing, weighing = route_tables(routes, route_weight, experts, slots)
    buffer = lax.dot_general(
        placing, moe_normed, (((0,), (0,)), ((), ())), preferred_element_type=jnp.float32
    )
    buffer = buffer.astype(jnp.bfloat16).reshape(experts, slots, -1)
    gate_shard = exp_gate[0]
    up_shard = exp_up[0]
    down_shard = exp_down[0]
    lanes = lax.axis_size("tp")
    small = experts <= 8 and lanes == 4
    if small:
        arrived, gathered, read, own = dispatch_pass(
            head_count, head_width, experts, lanes, buffer, *mix_operands
        )
    else:
        totals, read, own = local_pass(head_count, head_width, *mix_operands)
        arrived = lax.all_to_all(buffer, "ep", split_axis=0, concat_axis=0, tiled=True)
        both = lax.all_gather(totals[None], "ep", axis=0, tiled=True)
        owners = jnp.arange(experts)[:, None, None, None]
        gathered = jnp.where(owners < lax.axis_index("ep"), both[:, 0], both[:, 1])
    finish_operands = (gathered, read, own, out_gain[None], w_output)
    hidden = expert_hidden(arrived, gate_shard, up_shard)
    partial_sum = jnp.dot(
        hidden.reshape(-1, hidden.shape[-1]), down_shard, preferred_element_type=jnp.float32
    )
    partial_sum = partial_sum.reshape(experts, slots, -1).astype(jnp.bfloat16)
    if small:
        returned, mix_out = return_pass(
            head_count, head_width, experts, lanes, partial_sum, *finish_operands
        )
    else:
        where = lax.axis_index("ep").astype(jnp.int32)[None]
        partial_mix = finish_pass(head_count, head_width, where, *finish_operands)
        mix_out = lax.psum_scatter(partial_mix, "tp", scatter_dimension=0, tiled=True)
        summed = lax.psum_scatter(partial_sum, "tp", scatter_dimension=2, tiled=True)
        returned = lax.all_to_all(summed, "ep", split_axis=0, concat_axis=0, tiled=True)
    moe_out = jnp.dot(
        weighing, returned.reshape(experts * slots, -1), preferred_element_type=jnp.float32
    )
    return (mix_out, moe_out.astype(jnp.bfloat16))


def solution(mesh):
    return jax.shard_map(
        shards,
        mesh=mesh,
        in_specs=(
            P("ep", None),
            P(),
            P(None, "tp"),
            P(None, "tp"),
            P(None, "tp"),
            P(),
            P(None, "tp"),
            P(None, "tp"),
            P("tp"),
            P("tp"),
            P("ep", "tp"),
            P("tp"),
            P("tp", None),
            P("ep", None),
            P(),
            P("ep", None),
            P("ep", None),
            P("ep", None, "tp"),
            P("ep", None, "tp"),
            P("ep", "tp", None),
        ),
        out_specs=(P(("ep", "tp"), None), P("ep", "tp")),
        check_vma=False,
    )
```
